32 devices in a mesh: grp: 2 (over y), sp: 4 (over z), tp: 4 (over x, core).
Axes of the slice: x: 2, y: 2, z: 4, core: 2. Of those that a mesh axis runs over, the one named last changes fastest.
Arguments:
- layer_input: bfloat16 [4, 2048, 2048], P('grp', 'sp'), parts along dimension 0, may hold values from -6 to 6
- key_weight: bfloat16 [2048, 1024], P(None, 'tp'), may hold values from -0.125 to 0.125
- value_weight: bfloat16 [2048, 1024], P(None, 'tp'), may hold values from -0.125 to 0.125
- beta_weight: bfloat16 [2048, 8], replicated, may hold values from -0.125 to 0.125
- beta_shift: float32 [8], replicated
- decay_weight: bfloat16 [2048, 8], replicated, may hold values from -0.125 to 0.125
- decay_rate: float32 [8], replicated, may hold values from 0 to 0.05
- decay_extra: float32 [4, 2048, 8], P('grp', 'sp', 'tp'), parts along dimension 0, may hold values from -1.5 to 0
- query_new: bfloat16 [4, 1024], P('grp', 'tp'), parts along dimension 0, may hold values from -6 to 6
- gate_new: bfloat16 [4, 1024], P('grp', 'tp'), parts along dimension 0, may hold values from -6 to 6
- norm_gain: float32 [128], replicated, may hold values from 0.1 to 1.9
- out_weight: bfloat16 [8, 128, 2048], P('tp', 'sp'), may hold values from -0.1875 to 0.1875
Outputs:
- state_cache: bfloat16 [4, 8, 128, 128], P('grp', 'tp', None, 'sp'), parts along dimension 0
- read_out: float32 [4, 2048], P('grp', ('sp', 'tp')), parts along dimension 0
The draws below stay inside these ranges and needn't reach their ends.
There are 2 independent parts, one for each index of `grp`. The reference program is written for one: setup_inputs(seed, part) draws one part's arguments, and reference() takes and returns one part's arrays. A program takes and returns all parts, laid end to end along the dimension named above; an argument that names none is the same for every part. Nothing has to cross between parts.
All inputs are finite; a program needn't handle non-finite values.
Results may differ from the reference program's by a relative error of at most 0.013.
Values sent between devices are 32-bit elements; how exact they have to be, the bound alone decides.
A program may use at most 64 MiB of HBM per device.

```python
import math
import jax
import jax.numpy as jnp
from jax import lax

D = 2048
HEAD_TOTAL = 8
DK = 128
BLK = 64
PROMPT_TOTAL = 2
SEG = 512
PROMPT_LENGTH = 2048


def draw_decay_rate(key, part):
    first_key, second_key, third_key = jax.random.split(key, 3)
    head_order = jax.random.permutation(first_key, HEAD_TOTAL)
    slow_count = HEAD_TOTAL // 2
    slow_heads = head_order < slow_count
    fast_rate = jnp.exp(jax.random.uniform(second_key, (HEAD_TOTAL,), jnp.float32, math.log(0.0125), math.log(0.04)))
    slow_rate = jnp.exp(jax.random.uniform(third_key, (HEAD_TOTAL,), jnp.float32, math.log(0.05), math.log(0.2))) / PROMPT_LENGTH
    return jnp.where(slow_heads, slow_rate, fast_rate).astype(jnp.float32)


def draw_beta_shift(key, part):
    first_key = jax.random.fold_in(key, 0)
    head_order = jax.random.permutation(first_key, HEAD_TOTAL)
    slow_count = HEAD_TOTAL // 2
    slow_heads = head_order < slow_count
    fast_key, slow_key = jax.random.split(jax.random.fold_in(key, 7))
    fast_shift = jax.random.uniform(fast_key, (HEAD_TOTAL,), jnp.float32, -1.0, 1.0)
    slow_shift = jax.random.uniform(slow_key, (HEAD_TOTAL,), jnp.float32, math.log(0.06), math.log(0.2)) + math.log(DK / PROMPT_LENGTH)
    return jnp.where(slow_heads, slow_shift, fast_shift).astype(jnp.float32)


def draw_decay_extra(key, part):
    rate_key, position_random_key, length_random_key = jax.random.split(key, 3)
    segments = PROMPT_LENGTH // SEG
    segment_rate = jnp.exp(jax.random.uniform(rate_key, (PROMPT_TOTAL, segments, HEAD_TOTAL), jnp.float32, math.log(0.05), math.log(0.25))) / PROMPT_LENGTH
    drawn_level = jnp.repeat(segment_rate, SEG, axis=1)
    spike_position = jax.random.randint(position_random_key, (PROMPT_TOTAL, 2, HEAD_TOTAL), 0, PROMPT_LENGTH)
    spike_length = jax.random.uniform(length_random_key, (PROMPT_TOTAL, 2, HEAD_TOTAL), jnp.float32, 0.22, 0.5)
    token_positions = jnp.arange(PROMPT_LENGTH)
    spike_marks = (token_positions[None, None, :, None] == spike_position[:, :, None, :]).astype(jnp.float32)
    spike_groups = jnp.sum(spike_marks * spike_length[:, :, None, :], axis=1)
    return (-(drawn_level + spike_groups)).astype(jnp.float32)


def shard_levels(own_key, extent, cuts, low, largest):
    def one(axis_at, parts):
        draws = jax.random.uniform(jax.random.fold_in(jax.random.fold_in(own_key, 6), axis_at), (parts,), jnp.float32, low / len(cuts), largest / len(cuts))
        return jnp.repeat(jnp.exp(draws), extent[axis_at] // parts).reshape((-1,) + (1,) * (len(extent) - axis_at - 1))

    gain = one(*cuts[0])
    for cut in cuts[1:]:
        gain = gain * one(*cut)
    return gain


def centred(key, extent, deviation, most, cuts=(), kind=jnp.bfloat16):
    entries = jax.random.normal(key, extent, jnp.float32) * deviation
    if len(cuts) > 0:
        entries = shard_levels(key, extent, cuts, -0.22, 0.18) * entries
    return jnp.clip(entries, min=-most, max=most).astype(kind)


def setup_inputs(seed: int = 0, part: int = 0) -> dict:
    streams_of = jax.random.split(jax.random.key(seed), 13)
    part_keys = jax.random.split(jax.random.fold_in(streams_of[12], part), 13)
    layer_input = centred(part_keys[0], (PROMPT_TOTAL, PROMPT_LENGTH, D), 1.0, 6.0, ((1, 4),))
    key_weight = centred(streams_of[1], (D, HEAD_TOTAL * DK), D ** -0.5, 0.125, ((1, 4),))
    value_weight = centred(streams_of[2], (D, HEAD_TOTAL * DK), D ** -0.5, 0.125, ((1, 4),))
    beta_weight = centred(streams_of[3], (D, HEAD_TOTAL), D ** -0.5, 0.125)
    beta_shift = draw_beta_shift(jax.random.fold_in(streams_of[12], 71), part)
    decay_weight = centred(streams_of[5], (D, HEAD_TOTAL), D ** -0.5, 0.125)
    decay_rate = draw_decay_rate(jax.random.fold_in(streams_of[12], 71), part)
    decay_extra = draw_decay_extra(jax.random.fold_in(jax.random.fold_in(streams_of[12], part), 71), part)
    query_new = centred(part_keys[8], (PROMPT_TOTAL, HEAD_TOTAL * DK), 1.0, 6.0, ((1, 4),))
    gate_new = centred(part_keys[9], (PROMPT_TOTAL, HEAD_TOTAL * DK), 1.0, 6.0, ((1, 4),))
    norm_gain = jnp.clip(1.0 + 0.18 * jax.random.normal(streams_of[10], (DK,), jnp.float32), 0.1, 1.9)
    out_weight = centred(streams_of[11], (HEAD_TOTAL, DK, D), (HEAD_TOTAL * DK) ** -0.5, 0.1875, ((0, 4), (1, 4)))
    return dict(layer_input=layer_input, key_weight=key_weight, value_weight=value_weight, beta_weight=beta_weight, beta_shift=beta_shift, decay_weight=decay_weight, decay_rate=decay_rate, decay_extra=decay_extra, query_new=query_new, gate_new=gate_new, norm_gain=norm_gain, out_weight=out_weight)


epsilon = 1e-06
highest = lax.Precision.HIGHEST

def chain_states(key_rows, value_rows, beta, log_decay, span):
    seq_here, length, heads_here, head_size = key_rows.shape
    block_count = length // span
    unit_keys = key_rows * lax.rsqrt(lax.optimization_barrier(jnp.sum(key_rows * key_rows, axis=-1, keepdims=True)) + epsilon)

    def blocked(tensor):
        moved_axes = jnp.moveaxis(tensor, 2, 1)
        return moved_axes.reshape((seq_here, heads_here, block_count, span) + tensor.shape[3:])
    key_blocks = blocked(unit_keys)
    value_blocks = blocked(value_rows)
    beta_blocks = blocked(beta)
    cumulative = jnp.cumsum(blocked(log_decay), axis=-1)
    places = jnp.arange(span)
    strict = places[:, None] > places[None, :]
    weighted = key_blocks * beta_blocks[..., None]
    key_products = jnp.einsum('shnid,shnjd->shnij', weighted, key_blocks, precision=highest)
    spread = cumulative[..., :, None] - cumulative[..., None, :]
    lower_part = jnp.where(strict, key_products * jnp.exp(jnp.where(strict, spread, 0.0)), 0.0)
    system = jnp.eye(span, dtype=jnp.float32) + lower_part
    right_side = jnp.concatenate([value_blocks * beta_blocks[..., None], weighted * jnp.exp(cumulative)[..., None]], axis=-1)
    solved = jax.scipy.linalg.solve_triangular(system, right_side, lower=True)
    value_part = solved[..., :head_size]
    key_part = solved[..., head_size:]
    carried_keys = key_blocks * jnp.exp(cumulative[..., -1:] - cumulative)[..., None]
    block_decay = jnp.exp(cumulative[..., -1])
    sequence_in = tuple((jnp.moveaxis(tensor, 2, 0) for tensor in (value_part, key_part, carried_keys, block_decay)))

    def advance(carry_state, inputs):
        value_now, key_now, carried_now, decay_now = inputs
        fresh_values = value_now - jnp.einsum('shck,shkv->shcv', key_now, carry_state, precision=highest)
        carry_state = carry_state * decay_now[..., None, None] + jnp.einsum('shck,shcv->shkv', carried_now, fresh_values, precision=highest)
        return (carry_state, None)
    initial = jnp.zeros((seq_here, heads_here, head_size, head_size), jnp.float32)
    final_state, unused = lax.scan(advance, initial, sequence_in)
    return final_state

def reference(layer_input, key_weight, value_weight, beta_weight, beta_shift, decay_weight, decay_rate, decay_extra, query_new, gate_new, norm_gain, out_weight):
    seq_count, length, width = layer_input.shape
    key_rows = jnp.dot(layer_input.astype(jnp.float32), key_weight.astype(jnp.float32), preferred_element_type=jnp.float32).astype(jnp.bfloat16)
    value_rows = jnp.dot(layer_input.astype(jnp.float32), value_weight.astype(jnp.float32), preferred_element_type=jnp.float32).astype(jnp.bfloat16)
    beta_raw = jnp.dot(layer_input.astype(jnp.float32), beta_weight.astype(jnp.float32), preferred_element_type=jnp.float32).astype(jnp.bfloat16)
    decay_raw = jnp.dot(layer_input.astype(jnp.float32), decay_weight.astype(jnp.float32), preferred_element_type=jnp.float32).astype(jnp.bfloat16)
    beta = jax.nn.sigmoid(beta_raw.astype(jnp.float32) + beta_shift)
    log_decay = -decay_rate * jax.nn.softplus(decay_raw.astype(jnp.float32)) + decay_extra
    key_heads = key_rows.reshape(seq_count, length, HEAD_TOTAL, DK).astype(jnp.float32)
    value_heads = value_rows.reshape(seq_count, length, HEAD_TOTAL, DK).astype(jnp.float32)
    final_state = chain_states(key_heads, value_heads, beta, log_decay, BLK)
    state_cache = final_state.astype(jnp.bfloat16)
    query = query_new.reshape(seq_count, HEAD_TOTAL, DK).astype(jnp.float32)
    query = query * lax.rsqrt(lax.optimization_barrier(jnp.sum(query * query, axis=-1, keepdims=True)) + epsilon) * DK ** (-0.5)
    readout = jnp.einsum('shkv,shk->shv', final_state, query, precision=highest)
    scaled = readout * lax.rsqrt(lax.optimization_barrier(jnp.mean(readout * readout, axis=-1, keepdims=True)) + epsilon)
    gate_values = gate_new.reshape(seq_count, HEAD_TOTAL, DK).astype(jnp.float32)
    normed = (scaled * norm_gain * jax.nn.silu(gate_values)).astype(jnp.bfloat16)
    total = jnp.dot(normed.reshape(seq_count, HEAD_TOTAL * DK).astype(jnp.float32), out_weight.reshape(HEAD_TOTAL * DK, width).astype(jnp.float32), preferred_element_type=jnp.float32)
    return (state_cache, total)
```

```python
import functools

import jax
import jax.numpy as jnp
from jax import lax
from jax.experimental import pallas as pl
from jax.experimental.pallas import tpu as pltpu
from jax.sharding import PartitionSpec as P

DK = 128
SPAN = 128
MESH = pl.DeviceIdType.MESH

epsilon = 1e-06
highest = lax.Precision.HIGHEST
F32 = jnp.float32
BF16 = jnp.bfloat16
NN = (((1,), (0,)), ((), ()))
NT = (((1,), (1,)), ((), ()))
TN = (((0,), (0,)), ((), ()))


def mm(a, b, dims=NN, precision=None):
    return lax.dot_general(a, b, dims, precision=precision, preferred_element_type=F32)


def bf(a):
    return a.astype(BF16)


def split(a):
    high = bf(a)
    return high, bf(a - high.astype(F32))


def mm3(a, b, dims=NN):
    a_high, a_low = a
    b_high, b_low = b
    return mm(a_high, b_high, dims) + (mm(a_high, b_low, dims) + mm(a_low, b_high, dims))


def softplus(a):
    return jnp.maximum(a, 0.0) + jnp.log1p(jnp.exp(-jnp.abs(a)))


def row_of(scalars, width):
    lanes = lax.broadcasted_iota(jnp.int32, (1, width), 1)
    row = jnp.zeros((1, width), F32)
    for j in range(width):
        row = jnp.where(lanes == j, scalars[j], row)
    return row


def map_kernel(heads, rate_ref, shift_ref, x_ref, wk_ref, wv_ref, wb_ref, wd_ref, extra_ref, map_ref):
    length = x_ref.shape[1]
    head_total = wb_ref.shape[1]
    chunks = length // SPAN
    first = lax.axis_index("tp") * heads
    x = x_ref[0]
    kb = bf(mm(x, wk_ref[...]))
    vb = bf(mm(x, wv_ref[...]))
    beta_all = jax.nn.sigmoid(bf(mm(x, wb_ref[...])).astype(F32) + row_of(shift_ref, head_total))
    soft_all = softplus(bf(mm(x, wd_ref[...])).astype(F32)) * -row_of(rate_ref, head_total)
    head_lanes = lax.broadcasted_iota(jnp.int32, (length, head_total), 1)

    lanes = lax.broadcasted_iota(jnp.int32, (SPAN, SPAN), 1)
    rows = lax.broadcasted_iota(jnp.int32, (SPAN, SPAN), 0)
    strict = rows > lanes
    apart = rows ^ lanes
    eye = jnp.where(rows == lanes, 1.0, 0.0)
    tri = jnp.where(rows >= lanes, 1.0, 0.0)

    count = heads * chunks
    combos = [(h, n) for h in range(heads) for n in range(chunks)]
    log_matrix = jnp.zeros((SPAN, SPAN), F32)
    other = jnp.zeros((SPAN, SPAN), F32)
    betas, norms = [], []
    for h in range(heads):
        here = head_lanes == first + h
        beta = jnp.sum(jnp.where(here, beta_all, 0.0), axis=1, keepdims=True)
        log_decay = jnp.sum(jnp.where(here, soft_all, 0.0), axis=1, keepdims=True)
        log_decay = log_decay + extra_ref[0, :, h : h + 1]
        keys = kb[:, h * DK : (h + 1) * DK].astype(F32)
        inverse_norm = lax.rsqrt(jnp.sum(keys * keys, axis=1, keepdims=True) + epsilon)
        for n in range(chunks):
            c = h * chunks + n
            part = slice(n * SPAN, (n + 1) * SPAN)
            log_matrix = jnp.where(lanes == c, log_decay[part], log_matrix)
            other = jnp.where(lanes == count + c, beta[part], other)
            other = jnp.where(lanes == 2 * count + c, inverse_norm[part], other)
            betas.append(beta[part])
            norms.append(inverse_norm[part])
    cumulative = mm(tri, log_matrix, precision=highest)
    by_row = jnp.where(lanes < count, cumulative, other).T

    keys, lowers, inverses = [], [], []
    for c, (h, n) in enumerate(combos):
        kr = kb[n * SPAN : (n + 1) * SPAN, h * DK : (h + 1) * DK]
        spread = cumulative[:, c : c + 1] - by_row[c : c + 1]
        decay = jnp.exp(jnp.where(strict, spread, 0.0))
        scale = (betas[c] * norms[c]) * by_row[2 * count + c : 2 * count + c + 1]
        lower = jnp.where(strict, mm(kr, kr, NT) * scale * decay, 0.0)
        keys.append(kr)
        lowers.append(lower)
        inverses.append(eye - jnp.where(apart < 2, lower, 0.0))
    size = 2
    while size < SPAN:
        level = (apart >= size) & (apart < 2 * size)
        narrow = [bf(inverse) for inverse in inverses]
        steps = [mm(bf(jnp.where(level, lower, 0.0)), x1) for lower, x1 in zip(lowers, narrow)]
        inverses = [
            inverse - mm(x1, bf(step)) for inverse, x1, step in zip(inverses, narrow, steps)
        ]
        size *= 2

    decays, pieces = [], []
    for c, (h, n) in enumerate(combos):
        values = vb[n * SPAN : (n + 1) * SPAN, h * DK : (h + 1) * DK]
        last = cumulative[SPAN - 1 : SPAN, c : c + 1]
        beta_row = by_row[count + c : count + c + 1]
        key_row = beta_row * by_row[2 * count + c : 2 * count + c + 1] * jnp.exp(by_row[c : c + 1])
        carry = norms[c] * jnp.exp(last - cumulative[:, c : c + 1])
        key_part = mm(bf(inverses[c] * key_row), keys[c]) * carry
        value_part = mm(bf(inverses[c] * beta_row), values) * carry
        both = bf(jnp.concatenate([key_part, value_part], axis=1))
        pieces.append(mm(both, keys[c], TN))
        decays.append(jnp.exp(last))
    for h in range(heads):
        c = h * chunks
        key_map, offset = pieces[c][:DK], pieces[c][DK:]
        linear = eye * decays[c] - key_map
        for n in range(1, chunks):
            c = h * chunks + n
            key_map = bf(pieces[c][:DK])
            linear = linear * decays[c] - mm(bf(linear), key_map)
            offset = offset * decays[c] - mm(bf(offset), key_map) + pieces[c][DK:]
        map_ref[0, h, :DK] = linear
        map_ref[0, h, DK:] = offset


def chain_kernel(
    sp_size,
    tp_size,
    map_ref,
    query_ref,
    gate_ref,
    gain_ref,
    weight_ref,
    cache_ref,
    out_ref,
    state_in,
    state_out,
    cols_send,
    cols_recv,
    norm_send,
    norm_recv,
    part_send,
    part_recv,
    chain_send_sem,
    chain_recv_sem,
    cols_send_sem,
    cols_recv_sem,
    norm_send_sem,
    norm_recv_sem,
    part_send_sem,
    part_recv_sem,
):
    seqs, heads = map_ref.shape[:2]
    columns = weight_ref.shape[1]
    features = part_send.shape[2]
    devices = sp_size * tp_size
    last = sp_size - 1
    me = lax.axis_index("sp")
    tp_here = lax.axis_index("tp")
    rank = me * tp_size + tp_here
    unroll = devices <= 16

    def where(target):
        return {"sp": target // tp_size, "tp": target % tp_size}

    def each_other(body):
        def turn(step, carry):
            body(step, lax.rem(rank + step, devices))
            return carry

        lax.fori_loop(1, devices, turn, 0, unroll=unroll)

    barrier = pltpu.get_barrier_semaphore()
    each_other(
        lambda step, target: pl.semaphore_signal(
            barrier, inc=1, device_id=where(target), device_id_type=MESH
        )
    )
    pl.semaphore_wait(barrier, devices - 1)

    def chain_copy(p, target):
        return pltpu.make_async_remote_copy(
            src_ref=state_out.at[p],
            dst_ref=state_in.at[p],
            send_sem=chain_send_sem.at[p],
            recv_sem=chain_recv_sem.at[p],
            device_id={"sp": target},
            device_id_type=MESH,
        )

    def cols_copy(p, d):
        return pltpu.make_async_remote_copy(
            src_ref=cols_send.at[d, p],
            dst_ref=cols_recv.at[p],
            send_sem=cols_send_sem.at[d, p],
            recv_sem=cols_recv_sem.at[p],
            device_id={"sp": d},
            device_id_type=MESH,
        )

    def norm_copy(d):
        return pltpu.make_async_remote_copy(
            src_ref=norm_send,
            dst_ref=norm_recv,
            send_sem=norm_send_sem.at[d],
            recv_sem=norm_recv_sem,
            device_id={"sp": d},
            device_id_type=MESH,
        )

    @pl.when(me == last)
    def _():
        norm_send[...] = jnp.zeros_like(norm_send)

    queries = query_ref[...].astype(F32)
    gates = jax.nn.silu(gate_ref[...].astype(F32))
    for s in range(seqs):
        for h in range(heads):
            p = h * seqs + s

            @pl.when(me == 0)
            def _():
                state_out[p] = map_ref[s, h, DK:]

            @pl.when(me > 0)
            def _():
                linear = split(map_ref[s, h, :DK])
                chain_copy(p, 0).wait_recv()
                state_out[p] = mm3(split(state_in[p]), linear) + map_ref[s, h, DK:]

            @pl.when(me < last)
            def _():
                chain_copy(p, me + 1).start()

            @pl.when(me == last)
            def _():
                state = state_out[p]
                for d in range(sp_size):
                    cols_send[d, p] = state[d * columns : (d + 1) * columns]
                for d in range(last):
                    cols_copy(p, d).start()
                cols_recv[p] = state[last * columns :]
                query = queries[s : s + 1, h * DK : (h + 1) * DK]
                query = query * lax.rsqrt(
                    jnp.sum(query * query, axis=1, keepdims=True) + epsilon
                ) * DK ** (-0.5)
                readout = mm(query, state, NT, highest)
                mean = jnp.mean(readout * readout, axis=1, keepdims=True)
                scaled = readout * lax.rsqrt(mean + epsilon)
                gate = gates[s : s + 1, h * DK : (h + 1) * DK]
                norm_send[p : p + 1] = bf(scaled * gain_ref[...] * gate).astype(F32)

    @pl.when(me == last)
    def _():
        for d in range(last):
            norm_copy(d).start()
        norm_recv[...] = norm_send[...]

    @pl.when(me < last)
    def _():
        for p in range(seqs * heads):
            chain_copy(p, me + 1).wait_send()
        norm_copy(0).wait_recv()

    picked = (
        lax.broadcasted_iota(jnp.int32, (DK, columns), 0)
        == lax.broadcasted_iota(jnp.int32, (DK, columns), 1) + me * columns
    )
    normed = bf(mm(bf(norm_recv[...]), bf(jnp.where(picked, 1.0, 0.0))))
    partial = mm(normed[:seqs], weight_ref[0])
    for h in range(1, heads):
        partial = partial + mm(normed[h * seqs : (h + 1) * seqs], weight_ref[h])
    for j in range(devices):
        part_send[j] = partial[:, j * features : (j + 1) * features]

    def part_copy(step, target, slot):
        return pltpu.make_async_remote_copy(
            src_ref=part_send.at[target],
            dst_ref=part_recv.at[slot],
            send_sem=part_send_sem.at[step],
            recv_sem=part_recv_sem.at[slot],
            device_id=where(target),
            device_id_type=MESH,
        )

    each_other(lambda step, target: part_copy(step, target, rank).start())
    part_recv[rank] = part_send[rank]

    @pl.when(me < last)
    def _():
        for p in range(seqs * heads):
            cols_copy(p, 0).wait_recv()

    eye = bf(
        jnp.where(
            lax.broadcasted_iota(jnp.int32, (DK, DK), 0)
            == lax.broadcasted_iota(jnp.int32, (DK, DK), 1),
            1.0,
            0.0,
        )
    )
    for s in range(seqs):
        for h in range(heads):
            cache_ref[s, h] = bf(mm(eye, bf(cols_recv[h * seqs + s]), NT))

    each_other(lambda step, target: part_copy(step, target, target).wait_recv())

    def add(j, total):
        return total + part_recv[j]

    out_ref[...] = lax.fori_loop(0, devices, add, jnp.zeros(out_ref.shape, F32), unroll=unroll)

    each_other(lambda step, target: part_copy(step, target, rank).wait_send())

    @pl.when(me == last)
    def _():
        for d in range(last):
            norm_copy(d).wait_send()
            for p in range(seqs * heads):
                cols_copy(p, d).wait_send()


def per_device(
    sp_size,
    tp_size,
    layer_input,
    key_weight,
    value_weight,
    beta_weight,
    beta_shift,
    decay_weight,
    decay_rate,
    decay_extra,
    query_new,
    gate_new,
    norm_gain,
    out_weight,
):
    seqs, length, width = layer_input.shape
    heads = key_weight.shape[1] // DK
    columns = out_weight.shape[1]
    devices = sp_size * tp_size
    features = out_weight.shape[2] // devices
    pairs = seqs * heads
    norm_rows = -(-pairs // 8) * 8
    whole = lambda array: pl.BlockSpec(array.shape, lambda s: (0,) * array.ndim)
    smem = pl.BlockSpec(memory_space=pltpu.SMEM)
    vmem = pl.BlockSpec(memory_space=pltpu.VMEM)
    maps = pl.pallas_call(
        functools.partial(map_kernel, heads),
        grid=(seqs,),
        in_specs=[
            smem,
            smem,
            pl.BlockSpec((1, length, width), lambda s: (s, 0, 0)),
            whole(key_weight),
            whole(value_weight),
            whole(beta_weight),
            whole(decay_weight),
            pl.BlockSpec((1, length, heads), lambda s: (s, 0, 0)),
        ],
        out_specs=pl.BlockSpec((1, heads, 2 * DK, DK), lambda s: (s, 0, 0, 0)),
        out_shape=jax.ShapeDtypeStruct((seqs, heads, 2 * DK, DK), F32),
        compiler_params=pltpu.CompilerParams(vmem_limit_bytes=48 * 1024 * 1024),
    )(
        decay_rate,
        beta_shift,
        layer_input,
        key_weight,
        value_weight,
        beta_weight,
        decay_weight,
        decay_extra,
    )
    dma = pltpu.SemaphoreType.DMA
    return pl.pallas_call(
        functools.partial(chain_kernel, sp_size, tp_size),
        in_specs=[vmem] * 5,
        out_specs=(vmem, vmem),
        out_shape=(
            jax.ShapeDtypeStruct((seqs, heads, DK, columns), BF16),
            jax.ShapeDtypeStruct((seqs, features), F32),
        ),
        scratch_shapes=[
            pltpu.VMEM((pairs, DK, DK), F32),
            pltpu.VMEM((pairs, DK, DK), F32),
            pltpu.VMEM((sp_size, pairs, columns, DK), F32),
            pltpu.VMEM((pairs, columns, DK), F32),
            pltpu.VMEM((norm_rows, DK), F32),
            pltpu.VMEM((norm_rows, DK), F32),
            pltpu.VMEM((devices, seqs, features), F32),
            pltpu.VMEM((devices, seqs, features), F32),
            dma((pairs,)),
            dma((pairs,)),
            dma((sp_size, pairs)),
            dma((pairs,)),
            dma((sp_size,)),
            dma,
            dma((devices,)),
            dma((devices,)),
        ],
        compiler_params=pltpu.CompilerParams(collective_id=0, has_side_effects=True),
    )(maps, query_new, gate_new, norm_gain.reshape(1, DK), out_weight)


def solution(mesh):
    return jax.shard_map(
        functools.partial(per_device, mesh.shape["sp"], mesh.shape["tp"]),
        mesh=mesh,
        in_specs=(
            P("grp", "sp", None),
            P(None, "tp"),
            P(None, "tp"),
            P(),
            P(),
            P(),
            P(),
            P("grp", "sp", "tp"),
            P("grp", "tp"),
            P("grp", "tp"),
            P(),
            P("tp", "sp", None),
        ),
        out_specs=(P("grp", "tp", None, "sp"), P("grp", ("sp", "tp"))),
        check_vma=False,
    )
```

```python
import functools

import jax
import jax.numpy as jnp
from jax import lax
from jax.experimental import pallas as pl
from jax.experimental.pallas import tpu as pltpu
from jax.sharding import PartitionSpec as P

DK = 128
SPAN = 128
MESH = pl.DeviceIdType.MESH

epsilon = 1e-06
highest = lax.Precision.HIGHEST
F32 = jnp.float32
BF16 = jnp.bfloat16
NN = (((1,), (0,)), ((), ()))
NT = (((1,), (1,)), ((), ()))
TN = (((0,), (0,)), ((), ()))


def mm(a, b, dims=NN, precision=None):
    return lax.dot_general(a, b, dims, precision=precision, preferred_element_type=F32)


def bf(a):
    return a.astype(BF16)


def split(a):
    high = bf(a)
    return high, bf(a - high.astype(F32))


def mm3(a, b, dims=NN):
    a_high, a_low = a
    b_high, b_low = b
    return mm(a_high, b_high, dims) + (mm(a_high, b_low, dims) + mm(a_low, b_high, dims))


def softplus(a):
    return jnp.maximum(a, 0.0) + jnp.log1p(jnp.exp(-jnp.abs(a)))


def column_of(row):
    width = row.shape[1]
    rows = lax.broadcasted_iota(jnp.int32, (width, width), 0)
    lanes = lax.broadcasted_iota(jnp.int32, (width, width), 1)
    return jnp.sum(jnp.where(rows == lanes, row, 0.0), axis=1, keepdims=True)


def segment_maps(x, wk, wv, small_weights, rate_row, shift_row, extra, heads, first):
    length = x.shape[0]
    head_total = rate_row.shape[1]
    chunks = length // SPAN
    kb = bf(mm(x, wk))
    vb = bf(mm(x, wv))
    raw = bf(mm(small_weights, x, NT)).astype(F32)
    beta_all = jax.nn.sigmoid(raw[:head_total] + column_of(shift_row))
    soft_all = softplus(raw[head_total:]) * -column_of(rate_row)
    head_rows = lax.broadcasted_iota(jnp.int32, (head_total, length), 0)

    lanes = lax.broadcasted_iota(jnp.int32, (SPAN, SPAN), 1)
    rows = lax.broadcasted_iota(jnp.int32, (SPAN, SPAN), 0)
    strict = rows > lanes
    diagonal = rows == lanes
    apart = rows ^ lanes
    eye = jnp.where(diagonal, 1.0, 0.0)
    upper = jnp.where(rows <= lanes, 1.0, 0.0)

    combos = [(h, n) for h in range(heads) for n in range(chunks)]
    count = -(-len(combos) // 8) * 8
    places = lax.broadcasted_iota(jnp.int32, (count, SPAN), 0)
    logs = jnp.zeros((count, SPAN), F32)
    betas = jnp.zeros((count, SPAN), F32)
    norms = jnp.zeros((count, SPAN), F32)
    keys, products = [], []
    for h in range(heads):
        here = head_rows == first + h
        beta = jnp.sum(jnp.where(here, beta_all, 0.0), axis=0, keepdims=True)
        log_decay = jnp.sum(jnp.where(here, soft_all, 0.0), axis=0, keepdims=True)
        log_decay = log_decay + extra[h : h + 1]
        for n in range(chunks):
            c = h * chunks + n
            part = slice(n * SPAN, (n + 1) * SPAN)
            kr = kb[part, h * DK : (h + 1) * DK]
            product = mm(kr, kr, NT)
            squares = jnp.sum(jnp.where(diagonal, product, 0.0), axis=0, keepdims=True)
            logs = jnp.where(places == c, log_decay[:, part], logs)
            betas = jnp.where(places == c, beta[:, part], betas)
            norms = jnp.where(places == c, lax.rsqrt(squares + epsilon), norms)
            keys.append(kr)
            products.append(product)
    cumulative = mm(logs, upper, precision=highest)
    last_logs = cumulative[:, SPAN - 1 :]
    key_rows = betas * norms * jnp.exp(cumulative)
    carries = norms * jnp.exp(last_logs - cumulative)
    stacked = [cumulative, betas * norms, carries]
    if 3 * count < SPAN:
        stacked.append(jnp.zeros((SPAN - 3 * count, SPAN), F32))
    by_column = jnp.concatenate(stacked, axis=0).T
    block_decays = jnp.exp(last_logs)

    lowers, inverses = [], []
    for c in range(len(combos)):
        spread = by_column[:, c : c + 1] - cumulative[c : c + 1]
        scale = by_column[:, count + c : count + c + 1] * norms[c : c + 1]
        decay = jnp.exp(jnp.where(strict, spread, 0.0))
        lower = jnp.where(strict, products[c] * scale * decay, 0.0)
        lowers.append(lower)
        inverses.append(eye - jnp.where(apart < 2, lower, 0.0))
    size = 2
    while size < SPAN:
        level = (apart >= size) & (apart < 2 * size)
        narrow = [bf(inverse) for inverse in inverses]
        steps = [mm(bf(jnp.where(level, lower, 0.0)), x1) for lower, x1 in zip(lowers, narrow)]
        inverses = [
            inverse - mm(x1, bf(step)) for inverse, x1, step in zip(inverses, narrow, steps)
        ]
        size *= 2

    pieces = []
    for c, (h, n) in enumerate(combos):
        values = vb[n * SPAN : (n + 1) * SPAN, h * DK : (h + 1) * DK]
        carry = by_column[:, 2 * count + c : 2 * count + c + 1]
        key_part = mm(bf(inverses[c] * key_rows[c : c + 1]), keys[c]) * carry
        value_part = mm(bf(inverses[c] * betas[c : c + 1]), values) * carry
        both = bf(jnp.concatenate([key_part, value_part], axis=1))
        pieces.append(mm(both, keys[c], TN))
    maps = []
    for h in range(heads):
        c = h * chunks
        linear = eye * block_decays[c : c + 1] - pieces[c][:DK]
        offset = pieces[c][DK:]
        for n in range(1, chunks):
            c = h * chunks + n
            fading = block_decays[c : c + 1]
            key_map = bf(pieces[c][:DK])
            linear = linear * fading - mm(bf(linear), key_map)
            offset = offset * fading - mm(bf(offset), key_map) + pieces[c][DK:]
        maps.append((linear, offset))
    return maps


def mixer_kernel(
    sp_size,
    tp_size,
    x_hbm,
    wk_hbm,
    wv_hbm,
    wb_ref,
    wd_ref,
    shift_ref,
    rate_ref,
    extra_ref,
    query_ref,
    gate_ref,
    gain_ref,
    weight_ref,
    cache_ref,
    out_ref,
    x_ref,
    wk_ref,
    wv_ref,
    maps,
    state_in,
    state_out,
    cols_send,
    cols_recv,
    back_in,
    back_out,
    norm_send,
    norm_recv,
    part_send,
    part_recv,
    load_sem,
    chain_send_sem,
    chain_recv_sem,
    cols_send_sem,
    cols_recv_sem,
    back_sem,
    norm_send_sem,
    norm_recv_sem,
    part_send_sem,
    part_recv_sem,
):
    seqs, heads = maps.shape[:2]
    pairs = seqs * heads
    columns = weight_ref.shape[1]
    features = part_send.shape[2]
    devices = sp_size * tp_size
    last = sp_size - 1
    half = DK // 2
    me = lax.axis_index("sp")
    tp_here = lax.axis_index("tp")
    rank = me * tp_size + tp_here
    unroll = devices <= 16

    def where(target):
        return {"sp": target // tp_size, "tp": target % tp_size}

    def each_other(body):
        def turn(step, carry):
            body(step, lax.rem(rank + step, devices))
            return carry

        lax.fori_loop(1, devices, turn, 0, unroll=unroll)

    loads = [
        pltpu.make_async_copy(wk_hbm, wk_ref, load_sem.at[0]),
        pltpu.make_async_copy(wv_hbm, wv_ref, load_sem.at[1]),
    ]
    loads += [
        pltpu.make_async_copy(x_hbm.at[s], x_ref.at[s], load_sem.at[2 + s]) for s in range(seqs)
    ]
    for load in (loads[0], loads[2], loads[1], *loads[3:]):
        load.start()
    barrier = pltpu.get_barrier_semaphore()
    each_other(
        lambda step, target: pl.semaphore_signal(
            barrier, inc=1, device_id=where(target), device_id_type=MESH
        )
    )

    def chain_copy(p, t, target):
        return pltpu.make_async_remote_copy(
            src_ref=state_out.at[p, t],
            dst_ref=state_in.at[p, t],
            send_sem=chain_send_sem.at[p, t],
            recv_sem=chain_recv_sem.at[p, t],
            device_id={"sp": target},
            device_id_type=MESH,
        )

    def cols_copy(p, d):
        return pltpu.make_async_remote_copy(
            src_ref=cols_send.at[d, p],
            dst_ref=cols_recv.at[p],
            send_sem=cols_send_sem.at[d, p],
            recv_sem=cols_recv_sem.at[p],
            device_id={"sp": d},
            device_id_type=MESH,
        )

    def back_copy(target):
        return pltpu.make_async_remote_copy(
            src_ref=back_out,
            dst_ref=back_in,
            send_sem=back_sem.at[0],
            recv_sem=back_sem.at[1],
            device_id={"sp": target},
            device_id_type=MESH,
        )

    def norm_copy(d):
        return pltpu.make_async_remote_copy(
            src_ref=norm_send,
            dst_ref=norm_recv,
            send_sem=norm_send_sem.at[d],
            recv_sem=norm_recv_sem,
            device_id={"sp": d},
            device_id_type=MESH,
        )

    def part_copy(step, target, slot):
        return pltpu.make_async_remote_copy(
            src_ref=part_send.at[target],
            dst_ref=part_recv.at[slot],
            send_sem=part_send_sem.at[step],
            recv_sem=part_recv_sem.at[slot],
            device_id=where(target),
            device_id_type=MESH,
        )

    small_weights = jnp.concatenate([wb_ref[...], wd_ref[...]], axis=0)
    for load in (loads[0], loads[1]):
        load.wait()
    for s in range(seqs):
        loads[2 + s].wait()
        found = segment_maps(
            x_ref[s],
            wk_ref[...],
            wv_ref[...],
            small_weights,
            rate_ref[...],
            shift_ref[...],
            extra_ref[s],
            heads,
            tp_here * heads,
        )
        for h in range(heads):
            maps[s, h, :DK] = found[h][0]
            maps[s, h, DK:] = found[h][1]
        if s == 0:
            pl.semaphore_wait(barrier, devices - 1)

        @pl.when(me == 0)
        def _():
            for h in range(heads):
                p = s * heads + h
                for t in range(2):
                    state_out[p, t] = maps[s, h, DK + t * half : DK + (t + 1) * half]
                    chain_copy(p, t, 1).start()

    def back_step():
        @pl.when(me == last)
        def _():
            queries = query_ref[...].astype(F32)
            back_in[...] = jnp.zeros_like(back_in)
            for s in range(seqs):
                for h in range(heads):
                    query = queries[s : s + 1, h * DK : (h + 1) * DK]
                    size = jnp.sum(query * query, axis=1, keepdims=True) + epsilon
                    row = s * heads + h
                    back_in[0, row : row + 1] = query * lax.rsqrt(size) * DK ** (-0.5)

        @pl.when(me < last)
        def _():
            back_copy(0).wait_recv()

        for s in range(seqs):
            for h in range(heads):
                row = s * heads + h
                query = split(back_in[0, row : row + 1])
                moved = mm3(query, split(maps[s, h]), NT)
                back_out[0, row : row + 1] = moved[:, :DK]
                back_out[1, row : row + 1] = back_in[1, row : row + 1] + moved[:, DK:]

        @pl.when(me > 0)
        def _():
            back_copy(me - 1).start()

        @pl.when(me == 0)
        def _():
            gates = jax.nn.silu(gate_ref[...].astype(F32))
            norm_send[...] = jnp.zeros_like(norm_send)
            for s in range(seqs):
                for h in range(heads):
                    row = s * heads + h
                    readout = back_out[1, row : row + 1]
                    mean = jnp.mean(readout * readout, axis=1, keepdims=True)
                    scaled = readout * lax.rsqrt(mean + epsilon)
                    gate = gates[s : s + 1, h * DK : (h + 1) * DK]
                    to = h * seqs + s
                    norm_send[to : to + 1] = bf(scaled * gain_ref[...] * gate).astype(F32)
            for d in range(1, sp_size):
                norm_copy(d).start()
            norm_recv[...] = norm_send[...]

    def out_step():
        @pl.when(me > 0)
        def _():
            norm_copy(0).wait_recv()

        picked = (
            lax.broadcasted_iota(jnp.int32, (DK, columns), 0)
            == lax.broadcasted_iota(jnp.int32, (DK, columns), 1) + me * columns
        )
        normed = bf(mm(bf(norm_recv[...]), bf(jnp.where(picked, 1.0, 0.0))))
        partial = mm(normed[:seqs], weight_ref[0])
        for h in range(1, heads):
            partial = partial + mm(normed[h * seqs : (h + 1) * seqs], weight_ref[h])
        for j in range(devices):
            part_send[j] = partial[:, j * features : (j + 1) * features]
        each_other(lambda step, target: part_copy(step, target, rank).start())
        part_recv[rank] = part_send[rank]

    def state_steps(chosen):
        @pl.when(me > 0)
        def _():
            for p in chosen:
                s, h = divmod(p, heads)
                linear = split(maps[s, h, :DK])
                for t in range(2):
                    offset = maps[s, h, DK + t * half : DK + (t + 1) * half]
                    chain_copy(p, t, 0).wait_recv()
                    state = mm3(split(state_in[p, t]), linear) + offset
                    state_out[p, t] = state

                    @pl.when(me < last)
                    def _():
                        chain_copy(p, t, me + 1).start()

                    @pl.when(me == last)
                    def _():
                        for d in range(t * half // columns, (t + 1) * half // columns):
                            at = d * columns - t * half
                            if d == last:
                                cols_recv[p] = state[at : at + columns]
                            else:
                                cols_send[d, p] = state[at : at + columns]
                                cols_copy(p, d).start()

    middle = pairs // 2
    late = 2 * me >= sp_size

    @pl.when(late)
    def _():
        back_step()

    state_steps(range(middle))

    @pl.when(jnp.logical_not(late))
    def _():
        back_step()

    @pl.when(me == last)
    def _():
        out_step()

    state_steps(range(middle, pairs))

    @pl.when(me < last)
    def _():
        out_step()

    each_other(lambda step, target: part_copy(step, target, target).wait_recv())

    def add(j, total):
        return total + part_recv[j]

    out_ref[...] = lax.fori_loop(0, devices, add, jnp.zeros(out_ref.shape, F32), unroll=unroll)

    @pl.when(me < last)
    def _():
        for p in range(pairs):
            for t in range(2):
                chain_copy(p, t, me + 1).wait_send()
            cols_copy(p, 0).wait_recv()

    for p in range(pairs):
        s, h = divmod(p, heads)
        cache_ref[s, h] = cols_recv[p]

    each_other(lambda step, target: part_copy(step, target, rank).wait_send())

    @pl.when(me == last)
    def _():
        for d in range(last):
            for p in range(pairs):
                cols_copy(p, d).wait_send()

    @pl.when(me > 0)
    def _():
        back_copy(me - 1).wait_send()

    @pl.when(me == 0)
    def _():
        for d in range(1, sp_size):
            norm_copy(d).wait_send()


def finish_kernel(cache_ref, out_ref, cache_out, out_out):
    cache_out[...] = bf(cache_ref[...])
    out_out[...] = out_ref[...]


def per_device(
    sp_size,
    tp_size,
    layer_input,
    key_weight,
    value_weight,
    beta_weight,
    beta_shift,
    decay_weight,
    decay_rate,
    decay_extra,
    query_new,
    gate_new,
    norm_gain,
    out_weight,
):
    seqs = layer_input.shape[0]
    heads = key_weight.shape[1] // DK
    head_total = beta_weight.shape[1]
    columns = out_weight.shape[1]
    devices = sp_size * tp_size
    features = out_weight.shape[2] // devices
    pairs = seqs * heads
    rows = -(-pairs // 8) * 8
    vmem = pl.BlockSpec(memory_space=pltpu.VMEM)
    anywhere = pl.BlockSpec(memory_space=pl.ANY)
    dma = pltpu.SemaphoreType.DMA
    states = jax.ShapeDtypeStruct((seqs, heads, columns, DK), F32)
    outs = jax.ShapeDtypeStruct((seqs, features), F32)
    cache, out = pl.pallas_call(
        functools.partial(mixer_kernel, sp_size, tp_size),
        in_specs=[anywhere] * 3 + [vmem] * 9,
        out_specs=(vmem, vmem),
        out_shape=(states, outs),
        scratch_shapes=[
            pltpu.VMEM(layer_input.shape, BF16),
            pltpu.VMEM(key_weight.shape, BF16),
            pltpu.VMEM(value_weight.shape, BF16),
            pltpu.VMEM((seqs, heads, 2 * DK, DK), F32),
            pltpu.VMEM((pairs, 2, DK // 2, DK), F32),
            pltpu.VMEM((pairs, 2, DK // 2, DK), F32),
            pltpu.VMEM((sp_size, pairs, columns, DK), F32),
            pltpu.VMEM((pairs, columns, DK), F32),
            pltpu.VMEM((2, rows, DK), F32),
            pltpu.VMEM((2, rows, DK), F32),
            pltpu.VMEM((rows, DK), F32),
            pltpu.VMEM((rows, DK), F32),
            pltpu.VMEM((devices, seqs, features), F32),
            pltpu.VMEM((devices, seqs, features), F32),
            dma((2 + seqs,)),
            dma((pairs, 2)),
            dma((pairs, 2)),
            dma((sp_size, pairs)),
            dma((pairs,)),
            dma((2,)),
            dma((sp_size,)),
            dma,
            dma((devices,)),
            dma((devices,)),
        ],
        compiler_params=pltpu.CompilerParams(
            collective_id=0, has_side_effects=True, vmem_limit_bytes=62 * 1024 * 1024
        ),
    )(
        layer_input,
        key_weight,
        value_weight,
        beta_weight.T,
        decay_weight.T,
        beta_shift.reshape(1, head_total),
        decay_rate.reshape(1, head_total),
        jnp.swapaxes(decay_extra, 1, 2),
        query_new,
        gate_new,
        norm_gain.reshape(1, DK),
        out_weight,
    )
    cache, out = pl.pallas_call(
        finish_kernel,
        in_specs=[vmem] * 2,
        out_specs=(vmem, vmem),
        out_shape=(jax.ShapeDtypeStruct(states.shape, BF16), outs),
    )(cache, out)
    return (jnp.swapaxes(cache, 2, 3), out)


def solution(mesh):
    return jax.shard_map(
        functools.partial(per_device, mesh.shape["sp"], mesh.shape["tp"]),
        mesh=mesh,
        in_specs=(
            P("grp", "sp", None),
            P(None, "tp"),
            P(None, "tp"),
            P(),
            P(),
            P(),
            P(),
            P("grp", "sp", "tp"),
            P("grp", "tp"),
            P("grp", "tp"),
            P(),
            P("tp", "sp", None),
        ),
        out_specs=(P("grp", "tp", None, "sp"), P("grp", ("sp", "tp"))),
        check_vma=False,
    )
```

```python
import functools

import jax
import jax.numpy as jnp
from jax import lax
from jax.experimental import pallas as pl
from jax.experimental.pallas import tpu as pltpu
from jax.sharding import PartitionSpec as P

DK = 128
SPAN = 128
MESH = pl.DeviceIdType.MESH

epsilon = 1e-06
highest = lax.Precision.HIGHEST
F32 = jnp.float32
BF16 = jnp.bfloat16
NN = (((1,), (0,)), ((), ()))
NT = (((1,), (1,)), ((), ()))
TN = (((0,), (0,)), ((), ()))


def mm(a, b, dims=NN, precision=None):
    return lax.dot_general(a, b, dims, precision=precision, preferred_element_type=F32)


def bf(a):
    return a.astype(BF16)


def split(a):
    high = bf(a)
    return high, bf(a - high.astype(F32))


def mm3(a, b, dims=NN):
    a_high, a_low = a
    b_high, b_low = b
    return mm(a_high, b_high, dims) + (mm(a_high, b_low, dims) + mm(a_low, b_high, dims))


def softplus(a):
    return jnp.maximum(a, 0.0) + jnp.log1p(jnp.exp(-jnp.abs(a)))


def column_of(row):
    width = row.shape[1]
    rows = lax.broadcasted_iota(jnp.int32, (width, width), 0)
    lanes = lax.broadcasted_iota(jnp.int32, (width, width), 1)
    return jnp.sum(jnp.where(rows == lanes, row, 0.0), axis=1, keepdims=True)


def segment_maps(x, wk, wv, small_weights, rate_row, shift_row, extra, heads, first):
    length = x.shape[0]
    head_total = rate_row.shape[1]
    chunks = length // SPAN
    kb = bf(mm(x, wk))
    vb = bf(mm(x, wv))
    raw = bf(mm(small_weights, x, NT)).astype(F32)
    beta_all = jax.nn.sigmoid(raw[:head_total] + column_of(shift_row))
    soft_all = softplus(raw[head_total:]) * -column_of(rate_row)
    head_rows = lax.broadcasted_iota(jnp.int32, (head_total, length), 0)

    lanes = lax.broadcasted_iota(jnp.int32, (SPAN, SPAN), 1)
    rows = lax.broadcasted_iota(jnp.int32, (SPAN, SPAN), 0)
    strict = rows > lanes
    diagonal = rows == lanes
    apart = rows ^ lanes
    eye = jnp.where(diagonal, 1.0, 0.0)
    upper = jnp.where(rows <= lanes, 1.0, 0.0)

    combos = [(h, n) for h in range(heads) for n in range(chunks)]
    count = -(-len(combos) // 8) * 8
    places = lax.broadcasted_iota(jnp.int32, (count, SPAN), 0)
    logs = jnp.zeros((count, SPAN), F32)
    betas = jnp.zeros((count, SPAN), F32)
    norms = jnp.zeros((count, SPAN), F32)
    keys, products = [], []
    for h in range(heads):
        here = head_rows == first + h
        beta = jnp.sum(jnp.where(here, beta_all, 0.0), axis=0, keepdims=True)
        log_decay = jnp.sum(jnp.where(here, soft_all, 0.0), axis=0, keepdims=True)
        log_decay = log_decay + extra[h : h + 1]
        for n in range(chunks):
            c = h * chunks + n
            part = slice(n * SPAN, (n + 1) * SPAN)
            kr = kb[part, h * DK : (h + 1) * DK]
            product = mm(kr, kr, NT)
            squares = jnp.sum(jnp.where(diagonal, product, 0.0), axis=0, keepdims=True)
            logs = jnp.where(places == c, log_decay[:, part], logs)
            betas = jnp.where(places == c, beta[:, part], betas)
            norms = jnp.where(places == c, lax.rsqrt(squares + epsilon), norms)
            keys.append(kr)
            products.append(product)
    cumulative = mm(logs, upper, precision=highest)
    last_logs = cumulative[:, SPAN - 1 :]
    key_rows = betas * norms * jnp.exp(cumulative)
    carries = norms * jnp.exp(last_logs - cumulative)
    stacked = [cumulative, betas * norms, carries]
    if 3 * count < SPAN:
        stacked.append(jnp.zeros((SPAN - 3 * count, SPAN), F32))
    by_column = jnp.concatenate(stacked, axis=0).T
    block_decays = jnp.exp(last_logs)

    lowers, inverses = [], []
    for c in range(len(combos)):
        spread = by_column[:, c : c + 1] - cumulative[c : c + 1]
        scale = by_column[:, count + c : count + c + 1] * norms[c : c + 1]
        decay = jnp.exp(jnp.where(strict, spread, 0.0))
        lower = jnp.where(strict, products[c] * scale * decay, 0.0)
        lowers.append(lower)
        inverses.append(eye - jnp.where(apart < 2, lower, 0.0))
    size = 2
    while size < SPAN:
        level = (apart >= size) & (apart < 2 * size)
        narrow = [bf(inverse) for inverse in inverses]
        steps = [mm(bf(jnp.where(level, lower, 0.0)), x1) for lower, x1 in zip(lowers, narrow)]
        inverses = [
            inverse - mm(x1, bf(step)) for inverse, x1, step in zip(inverses, narrow, steps)
        ]
        size *= 2

    pieces = []
    for c, (h, n) in enumerate(combos):
        values = vb[n * SPAN : (n + 1) * SPAN, h * DK : (h + 1) * DK]
        carry = by_column[:, 2 * count + c : 2 * count + c + 1]
        key_part = mm(bf(inverses[c] * key_rows[c : c + 1]), keys[c]) * carry
        value_part = mm(bf(inverses[c] * betas[c : c + 1]), values) * carry
        both = bf(jnp.concatenate([key_part, value_part], axis=1))
        pieces.append(mm(both, keys[c], TN))
    maps = []
    for h in range(heads):
        c = h * chunks
        linear = eye * block_decays[c : c + 1] - pieces[c][:DK]
        offset = pieces[c][DK:]
        for n in range(1, chunks):
            c = h * chunks + n
            fading = block_decays[c : c + 1]
            key_map = bf(pieces[c][:DK])
            linear = linear * fading - mm(bf(linear), key_map)
            offset = offset * fading - mm(bf(offset), key_map) + pieces[c][DK:]
        maps.append((linear, offset))
    return maps


def mixer_kernel(
    sp_size,
    tp_size,
    x_hbm,
    wk_hbm,
    wv_hbm,
    wb_ref,
    wd_ref,
    shift_ref,
    rate_ref,
    extra_ref,
    query_ref,
    gate_ref,
    gain_ref,
    weight_ref,
    cache_ref,
    out_ref,
    x_ref,
    wk_ref,
    wv_ref,
    maps,
    state_in,
    state_out,
    cols_send,
    cols_recv,
    back_in,
    back_out,
    norm_send,
    norm_recv,
    part_send,
    part_recv,
    load_sem,
    chain_send_sem,
    chain_recv_sem,
    cols_send_sem,
    cols_recv_sem,
    back_sem,
    norm_send_sem,
    norm_recv_sem,
    part_send_sem,
    part_recv_sem,
):
    seqs, heads = maps.shape[:2]
    pairs = seqs * heads
    columns = weight_ref.shape[1]
    features = part_send.shape[2]
    devices = sp_size * tp_size
    last = sp_size - 1
    meeting = last // 2
    half = DK // 2
    me = lax.axis_index("sp")
    tp_here = lax.axis_index("tp")
    rank = me * tp_size + tp_here
    unroll = devices <= 16

    def where(target):
        return {"sp": target // tp_size, "tp": target % tp_size}

    def each_other(body):
        def turn(step, carry):
            body(step, lax.rem(rank + step, devices))
            return carry

        lax.fori_loop(1, devices, turn, 0, unroll=unroll)

    loads = [
        pltpu.make_async_copy(wk_hbm, wk_ref, load_sem.at[0]),
        pltpu.make_async_copy(wv_hbm, wv_ref, load_sem.at[1]),
    ]
    loads += [
        pltpu.make_async_copy(x_hbm.at[s], x_ref.at[s], load_sem.at[2 + s]) for s in range(seqs)
    ]
    for load in (loads[0], loads[2], loads[1], *loads[3:]):
        load.start()
    barrier = pltpu.get_barrier_semaphore()
    each_other(
        lambda step, target: pl.semaphore_signal(
            barrier, inc=1, device_id=where(target), device_id_type=MESH
        )
    )

    def chain_copy(p, t, target):
        return pltpu.make_async_remote_copy(
            src_ref=state_out.at[p, t],
            dst_ref=state_in.at[p, t],
            send_sem=chain_send_sem.at[p, t],
            recv_sem=chain_recv_sem.at[p, t],
            device_id={"sp": target},
            device_id_type=MESH,
        )

    def cols_copy(p, d):
        return pltpu.make_async_remote_copy(
            src_ref=cols_send.at[d, p],
            dst_ref=cols_recv.at[p],
            send_sem=cols_send_sem.at[d, p],
            recv_sem=cols_recv_sem.at[p],
            device_id={"sp": d},
            device_id_type=MESH,
        )

    def back_copy(target):
        return pltpu.make_async_remote_copy(
            src_ref=back_out,
            dst_ref=back_in,
            send_sem=back_sem.at[0],
            recv_sem=back_sem.at[1],
            device_id={"sp": target},
            device_id_type=MESH,
        )

    def norm_copy(d):
        return pltpu.make_async_remote_copy(
            src_ref=norm_send,
            dst_ref=norm_recv,
            send_sem=norm_send_sem.at[d],
            recv_sem=norm_recv_sem,
            device_id={"sp": d},
            device_id_type=MESH,
        )

    def part_copy(step, target, slot):
        return pltpu.make_async_remote_copy(
            src_ref=part_send.at[target],
            dst_ref=part_recv.at[slot],
            send_sem=part_send_sem.at[step],
            recv_sem=part_recv_sem.at[slot],
            device_id=where(target),
            device_id_type=MESH,
        )

    small_weights = jnp.concatenate([wb_ref[...], wd_ref[...]], axis=0)
    for load in (loads[0], loads[1]):
        load.wait()
    for s in range(seqs):
        loads[2 + s].wait()
        found = segment_maps(
            x_ref[s],
            wk_ref[...],
            wv_ref[...],
            small_weights,
            rate_ref[...],
            shift_ref[...],
            extra_ref[s],
            heads,
            tp_here * heads,
        )
        for h in range(heads):
            maps[s, h, :DK] = found[h][0]
            maps[s, h, DK:] = found[h][1]
        if s == 0:
            pl.semaphore_wait(barrier, devices - 1)

        @pl.when(me == 0)
        def _():
            for h in range(heads):
                p = s * heads + h
                for t in range(2):
                    state_out[p, t] = maps[s, h, DK + t * half : DK + (t + 1) * half]
                    chain_copy(p, t, 1).start()

    def back_step():
        @pl.when(me == last)
        def _():
            queries = query_ref[...].astype(F32)
            back_in[...] = jnp.zeros_like(back_in)
            for s in range(seqs):
                for h in range(heads):
                    query = queries[s : s + 1, h * DK : (h + 1) * DK]
                    size = jnp.sum(query * query, axis=1, keepdims=True) + epsilon
                    row = s * heads + h
                    back_in[0, row : row + 1] = query * lax.rsqrt(size) * DK ** (-0.5)

        @pl.when(me < last)
        def _():
            back_copy(0).wait_recv()

        @pl.when(me > meeting)
        def _():
            moves = []
            for s in range(seqs):
                for h in range(heads):
                    row = s * heads + h
                    moves.append(mm3(split(back_in[0, row : row + 1]), split(maps[s, h]), NT))
            for row, moved in enumerate(moves):
                back_out[0, row : row + 1] = moved[:, :DK]
                back_out[1, row : row + 1] = back_in[1, row : row + 1] + moved[:, DK:]
            back_copy(me - 1).start()

        @pl.when(me == meeting)
        def _():
            reads = []
            for row in range(pairs):
                query = split(back_in[0, row : row + 1])
                reads.append([mm3(query, split(state_out[row, t]), NT) for t in range(2)])
            gates = jax.nn.silu(gate_ref[...].astype(F32))
            norm_send[...] = jnp.zeros_like(norm_send)
            for s in range(seqs):
                for h in range(heads):
                    row = s * heads + h
                    readout = back_in[1, row : row + 1] + jnp.concatenate(reads[row], axis=1)
                    mean = jnp.mean(readout * readout, axis=1, keepdims=True)
                    scaled = readout * lax.rsqrt(mean + epsilon)
                    gate = gates[s : s + 1, h * DK : (h + 1) * DK]
                    to = h * seqs + s
                    norm_send[to : to + 1] = bf(scaled * gain_ref[...] * gate).astype(F32)
            for d in range(sp_size):
                if d != meeting:
                    norm_copy(d).start()
            norm_recv[...] = norm_send[...]

    def out_step():
        @pl.when(me != meeting)
        def _():
            norm_copy(0).wait_recv()

        picked = (
            lax.broadcasted_iota(jnp.int32, (DK, columns), 0)
            == lax.broadcasted_iota(jnp.int32, (DK, columns), 1) + me * columns
        )
        normed = bf(mm(bf(norm_recv[...]), bf(jnp.where(picked, 1.0, 0.0))))
        partial = mm(normed[:seqs], weight_ref[0])
        for h in range(1, heads):
            partial = partial + mm(normed[h * seqs : (h + 1) * seqs], weight_ref[h])
        for j in range(devices):
            part_send[j] = partial[:, j * features : (j + 1) * features]
        each_other(lambda step, target: part_copy(step, target, rank).start())
        part_recv[rank] = part_send[rank]

    def state_steps(chosen):
        @pl.when(me > 0)
        def _():
            for p in chosen:
                s, h = divmod(p, heads)
                linear = split(maps[s, h, :DK])
                for t in range(2):
                    offset = maps[s, h, DK + t * half : DK + (t + 1) * half]
                    chain_copy(p, t, 0).wait_recv()
                    state = mm3(split(state_in[p, t]), linear) + offset
                    state_out[p, t] = state

                    @pl.when(me < last)
                    def _():
                        chain_copy(p, t, me + 1).start()

                    @pl.when(me == last)
                    def _():
                        for d in range(t * half // columns, (t + 1) * half // columns):
                            at = d * columns - t * half
                            if d == last:
                                cols_recv[p] = state[at : at + columns]
                            else:
                                cols_send[d, p] = state[at : at + columns]
                                cols_copy(p, d).start()

    @pl.when(me > meeting)
    def _():
        back_step()

    state_steps(range(pairs))

    @pl.when(me == meeting)
    def _():
        back_step()

    out_step()

    each_other(lambda step, target: part_copy(step, target, target).wait_recv())

    def add(j, total):
        return total + part_recv[j]

    out_ref[...] = lax.fori_loop(0, devices, add, jnp.zeros(out_ref.shape, F32), unroll=unroll)

    @pl.when(me < last)
    def _():
        for p in range(pairs):
            for t in range(2):
                chain_copy(p, t, me + 1).wait_send()
            cols_copy(p, 0).wait_recv()

    for p in range(pairs):
        s, h = divmod(p, heads)
        cache_ref[s, h] = cols_recv[p]

    each_other(lambda step, target: part_copy(step, target, rank).wait_send())

    @pl.when(me == last)
    def _():
        for d in range(last):
            for p in range(pairs):
                cols_copy(p, d).wait_send()

    @pl.when(me > meeting)
    def _():
        back_copy(me - 1).wait_send()

    @pl.when(me == meeting)
    def _():
        for d in range(sp_size):
            if d != meeting:
                norm_copy(d).wait_send()


def finish_kernel(cache_ref, out_ref, cache_out, out_out):
    cache_out[...] = bf(cache_ref[...])
    out_out[...] = out_ref[...]


def per_device(
    sp_size,
    tp_size,
    layer_input,
    key_weight,
    value_weight,
    beta_weight,
    beta_shift,
    decay_weight,
    decay_rate,
    decay_extra,
    query_new,
    gate_new,
    norm_gain,
    out_weight,
):
    seqs = layer_input.shape[0]
    heads = key_weight.shape[1] // DK
    head_total = beta_weight.shape[1]
    columns = out_weight.shape[1]
    devices = sp_size * tp_size
    features = out_weight.shape[2] // devices
    pairs = seqs * heads
    rows = -(-pairs // 8) * 8
    vmem = pl.BlockSpec(memory_space=pltpu.VMEM)
    anywhere = pl.BlockSpec(memory_space=pl.ANY)
    dma = pltpu.SemaphoreType.DMA
    states = jax.ShapeDtypeStruct((seqs, heads, columns, DK), F32)
    outs = jax.ShapeDtypeStruct((seqs, features), F32)
    cache, out = pl.pallas_call(
        functools.partial(mixer_kernel, sp_size, tp_size),
        in_specs=[anywhere] * 3 + [vmem] * 9,
        out_specs=(vmem, vmem),
        out_shape=(states, outs),
        scratch_shapes=[
            pltpu.VMEM(layer_input.shape, BF16),
            pltpu.VMEM(key_weight.shape, BF16),
            pltpu.VMEM(value_weight.shape, BF16),
            pltpu.VMEM((seqs, heads, 2 * DK, DK), F32),
            pltpu.VMEM((pairs, 2, DK // 2, DK), F32),
            pltpu.VMEM((pairs, 2, DK // 2, DK), F32),
            pltpu.VMEM((sp_size, pairs, columns, DK), F32),
            pltpu.VMEM((pairs, columns, DK), F32),
            pltpu.VMEM((2, rows, DK), F32),
            pltpu.VMEM((2, rows, DK), F32),
            pltpu.VMEM((rows, DK), F32),
            pltpu.VMEM((rows, DK), F32),
            pltpu.VMEM((devices, seqs, features), F32),
            pltpu.VMEM((devices, seqs, features), F32),
            dma((2 + seqs,)),
            dma((pairs, 2)),
            dma((pairs, 2)),
            dma((sp_size, pairs)),
            dma((pairs,)),
            dma((2,)),
            dma((sp_size,)),
            dma,
            dma((devices,)),
            dma((devices,)),
        ],
        compiler_params=pltpu.CompilerParams(
            collective_id=0, has_side_effects=True, vmem_limit_bytes=62 * 1024 * 1024
        ),
    )(
        layer_input,
        key_weight,
        value_weight,
        beta_weight.T,
        decay_weight.T,
        beta_shift.reshape(1, head_total),
        decay_rate.reshape(1, head_total),
        jnp.swapaxes(decay_extra, 1, 2),
        query_new,
        gate_new,
        norm_gain.reshape(1, DK),
        out_weight,
    )
    cache, out = pl.pallas_call(
        finish_kernel,
        in_specs=[vmem] * 2,
        out_specs=(vmem, vmem),
        out_shape=(jax.ShapeDtypeStruct(states.shape, BF16), outs),
    )(cache, out)
    return (jnp.swapaxes(cache, 2, 3), out)


def solution(mesh):
    return jax.shard_map(
        functools.partial(per_device, mesh.shape["sp"], mesh.shape["tp"]),
        mesh=mesh,
        in_specs=(
            P("grp", "sp", None),
            P(None, "tp"),
            P(None, "tp"),
            P(),
            P(),
            P(),
            P(),
            P("grp", "sp", "tp"),
            P("grp", "tp"),
            P("grp", "tp"),
            P(),
            P("tp", "sp", None),
        ),
        out_specs=(P("grp", "tp", None, "sp"), P("grp", ("sp", "tp"))),
        check_vma=False,
    )
```

```python
import functools

import jax
import jax.numpy as jnp
from jax import lax
from jax.experimental import pallas as pl
from jax.experimental.pallas import tpu as pltpu
from jax.sharding import PartitionSpec as P

DK = 128
SPAN = 128
MESH = pl.DeviceIdType.MESH

epsilon = 1e-06
highest = lax.Precision.HIGHEST
F32 = jnp.float32
BF16 = jnp.bfloat16
NN = (((1,), (0,)), ((), ()))
NT = (((1,), (1,)), ((), ()))
TN = (((0,), (0,)), ((), ()))


def mm(a, b, dims=NN, precision=None):
    return lax.dot_general(a, b, dims, precision=precision, preferred_element_type=F32)


def bf(a):
    return a.astype(BF16)


def split(a):
    high = bf(a)
    return high, bf(a - high.astype(F32))


def mm3(a, b, dims=NN):
    a_high, a_low = a
    b_high, b_low = b
    return mm(a_high, b_high, dims) + (mm(a_high, b_low, dims) + mm(a_low, b_high, dims))


def softplus(a):
    return jnp.maximum(a, 0.0) + jnp.log1p(jnp.exp(-jnp.abs(a)))


def column_of(row):
    width = row.shape[1]
    rows = lax.broadcasted_iota(jnp.int32, (width, width), 0)
    lanes = lax.broadcasted_iota(jnp.int32, (width, width), 1)
    return jnp.sum(jnp.where(rows == lanes, row, 0.0), axis=1, keepdims=True)


def segment_maps(x, wk, wv, small_weights, rate_row, shift_row, extra, heads, first):
    length = x.shape[0]
    head_total = rate_row.shape[1]
    chunks = length // SPAN
    kb = bf(mm(x, wk))
    vb = bf(mm(x, wv))
    raw = bf(mm(small_weights, x, NT)).astype(F32)
    beta_all = jax.nn.sigmoid(raw[:head_total] + column_of(shift_row))
    soft_all = softplus(raw[head_total:]) * -column_of(rate_row)
    head_rows = lax.broadcasted_iota(jnp.int32, (head_total, length), 0)

    lanes = lax.broadcasted_iota(jnp.int32, (SPAN, SPAN), 1)
    rows = lax.broadcasted_iota(jnp.int32, (SPAN, SPAN), 0)
    strict = rows > lanes
    diagonal = rows == lanes
    apart = rows ^ lanes
    eye = jnp.where(diagonal, 1.0, 0.0)
    upper = jnp.where(rows <= lanes, 1.0, 0.0)

    combos = [(h, n) for h in range(heads) for n in range(chunks)]
    count = -(-len(combos) // 8) * 8
    places = lax.broadcasted_iota(jnp.int32, (count, SPAN), 0)
    logs = jnp.zeros((count, SPAN), F32)
    betas = jnp.zeros((count, SPAN), F32)
    norms = jnp.zeros((count, SPAN), F32)
    keys, products = [], []
    for h in range(heads):
        here = head_rows == first + h
        beta = jnp.sum(jnp.where(here, beta_all, 0.0), axis=0, keepdims=True)
        log_decay = jnp.sum(jnp.where(here, soft_all, 0.0), axis=0, keepdims=True)
        log_decay = log_decay + extra[h : h + 1]
        for n in range(chunks):
            c = h * chunks + n
            part = slice(n * SPAN, (n + 1) * SPAN)
            kr = kb[part, h * DK : (h + 1) * DK]
            product = mm(kr, kr, NT)
            squares = jnp.sum(jnp.where(diagonal, product, 0.0), axis=0, keepdims=True)
            logs = jnp.where(places == c, log_decay[:, part], logs)
            betas = jnp.where(places == c, beta[:, part], betas)
            norms = jnp.where(places == c, lax.rsqrt(squares + epsilon), norms)
            keys.append(kr)
            products.append(product)
    cumulative = mm(logs, upper, precision=highest)
    last_logs = cumulative[:, SPAN - 1 :]
    key_rows = betas * norms * jnp.exp(cumulative)
    carries = norms * jnp.exp(last_logs - cumulative)
    stacked = [cumulative, betas * norms, carries]
    if 3 * count < SPAN:
        stacked.append(jnp.zeros((SPAN - 3 * count, SPAN), F32))
    by_column = jnp.concatenate(stacked, axis=0).T
    block_decays = jnp.exp(last_logs)

    lowers, inverses = [], []
    for c in range(len(combos)):
        spread = by_column[:, c : c + 1] - cumulative[c : c + 1]
        scale = by_column[:, count + c : count + c + 1] * norms[c : c + 1]
        decay = jnp.exp(jnp.where(strict, spread, 0.0))
        lower = jnp.where(strict, products[c] * scale * decay, 0.0)
        lowers.append(lower)
        inverses.append(eye - jnp.where(apart < 2, lower, 0.0))
    size = 2
    while size < SPAN:
        level = (apart >= size) & (apart < 2 * size)
        narrow = [bf(inverse) for inverse in inverses]
        steps = [mm(bf(jnp.where(level, lower, 0.0)), x1) for lower, x1 in zip(lowers, narrow)]
        inverses = [
            inverse - mm(x1, bf(step)) for inverse, x1, step in zip(inverses, narrow, steps)
        ]
        size *= 2

    pieces = []
    for c, (h, n) in enumerate(combos):
        values = vb[n * SPAN : (n + 1) * SPAN, h * DK : (h + 1) * DK]
        carry = by_column[:, 2 * count + c : 2 * count + c + 1]
        key_part = mm(bf(inverses[c] * key_rows[c : c + 1]), keys[c]) * carry
        value_part = mm(bf(inverses[c] * betas[c : c + 1]), values) * carry
        both = bf(jnp.concatenate([key_part, value_part], axis=1))
        pieces.append(mm(both, keys[c], TN))
    maps = []
    for h in range(heads):
        c = h * chunks
        linear = eye * block_decays[c : c + 1] - pieces[c][:DK]
        offset = pieces[c][DK:]
        for n in range(1, chunks):
            c = h * chunks + n
            fading = block_decays[c : c + 1]
            key_map = bf(pieces[c][:DK])
            linear = linear * fading - mm(bf(linear), key_map)
            offset = offset * fading - mm(bf(offset), key_map) + pieces[c][DK:]
        maps.append((linear, offset))
    return maps


def mixer_kernel(
    sp_size,
    tp_size,
    x_hbm,
    wk_hbm,
    wv_hbm,
    wb_ref,
    wd_ref,
    shift_ref,
    rate_ref,
    extra_ref,
    query_ref,
    gate_ref,
    gain_ref,
    weight_ref,
    cache_ref,
    out_ref,
    x_ref,
    wk_ref,
    wv_ref,
    maps,
    state_in,
    state_out,
    cols_send,
    cols_recv,
    back_in,
    back_out,
    norm_send,
    norm_recv,
    part_send,
    part_recv,
    peer_maps,
    load_sem,
    chain_send_sem,
    chain_recv_sem,
    cols_send_sem,
    cols_recv_sem,
    back_sem,
    norm_send_sem,
    norm_recv_sem,
    part_send_sem,
    part_recv_sem,
    peer_send_sem,
    peer_recv_sem,
):
    seqs, heads = maps.shape[:2]
    pairs = seqs * heads
    columns = weight_ref.shape[1]
    features = part_send.shape[2]
    devices = sp_size * tp_size
    last = sp_size - 1
    meeting = last // 2
    half = DK // 2
    ends = [last] * pairs
    if sp_size > 2:
        for p in range(seqs // 2 * heads, pairs):
            ends[p] = last - 1
    me = lax.axis_index("sp")
    tp_here = lax.axis_index("tp")
    rank = me * tp_size + tp_here
    unroll = devices <= 16

    def where(target):
        return {"sp": target // tp_size, "tp": target % tp_size}

    def each_other(body):
        def turn(step, carry):
            body(step, lax.rem(rank + step, devices))
            return carry

        lax.fori_loop(1, devices, turn, 0, unroll=unroll)

    loads = [
        pltpu.make_async_copy(wk_hbm, wk_ref, load_sem.at[0]),
        pltpu.make_async_copy(wv_hbm, wv_ref, load_sem.at[1]),
    ]
    loads += [
        pltpu.make_async_copy(x_hbm.at[s], x_ref.at[s], load_sem.at[2 + s]) for s in range(seqs)
    ]
    for load in (loads[0], loads[2], loads[1], *loads[3:]):
        load.start()
    barrier = pltpu.get_barrier_semaphore()
    each_other(
        lambda step, target: pl.semaphore_signal(
            barrier, inc=1, device_id=where(target), device_id_type=MESH
        )
    )

    def chain_copy(p, t, target):
        return pltpu.make_async_remote_copy(
            src_ref=state_out.at[p, t],
            dst_ref=state_in.at[p, t],
            send_sem=chain_send_sem.at[p, t],
            recv_sem=chain_recv_sem.at[p, t],
            device_id={"sp": target},
            device_id_type=MESH,
        )

    def cols_copy(p, d):
        return pltpu.make_async_remote_copy(
            src_ref=cols_send.at[d, p],
            dst_ref=cols_recv.at[p],
            send_sem=cols_send_sem.at[d, p],
            recv_sem=cols_recv_sem.at[p],
            device_id={"sp": d},
            device_id_type=MESH,
        )

    def back_copy(target):
        return pltpu.make_async_remote_copy(
            src_ref=back_out,
            dst_ref=back_in,
            send_sem=back_sem.at[0],
            recv_sem=back_sem.at[1],
            device_id={"sp": target},
            device_id_type=MESH,
        )

    def norm_copy(d):
        return pltpu.make_async_remote_copy(
            src_ref=norm_send,
            dst_ref=norm_recv,
            send_sem=norm_send_sem.at[d],
            recv_sem=norm_recv_sem,
            device_id={"sp": d},
            device_id_type=MESH,
        )

    def peer_copy(p):
        s, h = divmod(p, heads)
        return pltpu.make_async_remote_copy(
            src_ref=maps.at[s, h],
            dst_ref=peer_maps.at[s, h],
            send_sem=peer_send_sem.at[p],
            recv_sem=peer_recv_sem.at[p],
            device_id={"sp": last - 1},
            device_id_type=MESH,
        )

    def part_copy(step, target, slot):
        return pltpu.make_async_remote_copy(
            src_ref=part_send.at[target],
            dst_ref=part_recv.at[slot],
            send_sem=part_send_sem.at[step],
            recv_sem=part_recv_sem.at[slot],
            device_id=where(target),
            device_id_type=MESH,
        )

    small_weights = jnp.concatenate([wb_ref[...], wd_ref[...]], axis=0)
    for load in (loads[0], loads[1]):
        load.wait()
    for s in range(seqs):
        loads[2 + s].wait()
        found = segment_maps(
            x_ref[s],
            wk_ref[...],
            wv_ref[...],
            small_weights,
            rate_ref[...],
            shift_ref[...],
            extra_ref[s],
            heads,
            tp_here * heads,
        )
        for h in range(heads):
            maps[s, h, :DK] = found[h][0]
            maps[s, h, DK:] = found[h][1]
        if s == 0:
            pl.semaphore_wait(barrier, devices - 1)

        @pl.when(me == 0)
        def _():
            for h in range(heads):
                p = s * heads + h
                for t in range(2):
                    state_out[p, t] = maps[s, h, DK + t * half : DK + (t + 1) * half]
                    chain_copy(p, t, 1).start()

    def back_step():
        @pl.when(me == last)
        def _():
            queries = query_ref[...].astype(F32)
            back_in[...] = jnp.zeros_like(back_in)
            for s in range(seqs):
                for h in range(heads):
                    query = queries[s : s + 1, h * DK : (h + 1) * DK]
                    size = jnp.sum(query * query, axis=1, keepdims=True) + epsilon
                    row = s * heads + h
                    back_in[0, row : row + 1] = query * lax.rsqrt(size) * DK ** (-0.5)

        @pl.when(me < last)
        def _():
            back_copy(0).wait_recv()

        @pl.when(me > meeting)
        def _():
            moves = []
            for s in range(seqs):
                for h in range(heads):
                    row = s * heads + h
                    moves.append(mm3(split(back_in[0, row : row + 1]), split(maps[s, h]), NT))
            for row, moved in enumerate(moves):
                back_out[0, row : row + 1] = moved[:, :DK]
                back_out[1, row : row + 1] = back_in[1, row : row + 1] + moved[:, DK:]
            back_copy(me - 1).start()

        @pl.when(me == meeting)
        def _():
            reads = []
            for row in range(pairs):
                query = split(back_in[0, row : row + 1])
                reads.append([mm3(query, split(state_out[row, t]), NT) for t in range(2)])
            gates = jax.nn.silu(gate_ref[...].astype(F32))
            norm_send[...] = jnp.zeros_like(norm_send)
            for s in range(seqs):
                for h in range(heads):
                    row = s * heads + h
                    readout = back_in[1, row : row + 1] + jnp.concatenate(reads[row], axis=1)
                    mean = jnp.mean(readout * readout, axis=1, keepdims=True)
                    scaled = readout * lax.rsqrt(mean + epsilon)
                    gate = gates[s : s + 1, h * DK : (h + 1) * DK]
                    to = h * seqs + s
                    norm_send[to : to + 1] = bf(scaled * gain_ref[...] * gate).astype(F32)
            for d in range(sp_size):
                if d != meeting:
                    norm_copy(d).start()
            norm_recv[...] = norm_send[...]

    def out_step():
        @pl.when(me != meeting)
        def _():
            norm_copy(0).wait_recv()

        picked = (
            lax.broadcasted_iota(jnp.int32, (DK, columns), 0)
            == lax.broadcasted_iota(jnp.int32, (DK, columns), 1) + me * columns
        )
        normed = bf(mm(bf(norm_recv[...]), bf(jnp.where(picked, 1.0, 0.0))))
        partial = mm(normed[:seqs], weight_ref[0])
        for h in range(1, heads):
            partial = partial + mm(normed[h * seqs : (h + 1) * seqs], weight_ref[h])
        for j in range(devices):
            part_send[j] = partial[:, j * features : (j + 1) * features]
        each_other(lambda step, target: part_copy(step, target, rank).start())
        part_recv[rank] = part_send[rank]

    def scatter(p, t, state):
        for d in range(t * half // columns, (t + 1) * half // columns):
            at = d * columns - t * half
            if d == ends[p]:
                cols_recv[p] = state[at : at + columns]
            else:
                cols_send[d, p] = state[at : at + columns]
                cols_copy(p, d).start()

    def state_step(p):
        s, h = divmod(p, heads)
        linear = split(maps[s, h, :DK])
        for t in range(2):
            rows_here = slice(DK + t * half, DK + (t + 1) * half)
            chain_copy(p, t, 0).wait_recv()
            state = mm3(split(state_in[p, t]), linear) + maps[s, h, rows_here]
            state_out[p, t] = state

            @pl.when(me < ends[p])
            def _():
                chain_copy(p, t, me + 1).start()

            @pl.when(me == ends[p])
            def _():
                if ends[p] == last:
                    scatter(p, t, state)
                else:
                    if t == 0:
                        peer_copy(p).wait_recv()
                    ahead = split(peer_maps[s, h, :DK])
                    scatter(p, t, mm3(split(state), ahead) + peer_maps[s, h, rows_here])

    @pl.when(me > meeting)
    def _():
        back_step()

    peers = [p for p in range(pairs) if ends[p] < last]

    @pl.when(me == last)
    def _():
        for p in peers:
            peer_copy(p).start()

    for p in range(pairs):

        @pl.when((me > 0) & (me <= ends[p]))
        def _():
            state_step(p)

    @pl.when(me == meeting)
    def _():
        back_step()

    out_step()

    each_other(lambda step, target: part_copy(step, target, target).wait_recv())

    def add(j, total):
        return total + part_recv[j]

    out_ref[...] = lax.fori_loop(0, devices, add, jnp.zeros(out_ref.shape, F32), unroll=unroll)

    for p in range(pairs):

        @pl.when(me < ends[p])
        def _():
            for t in range(2):
                chain_copy(p, t, me + 1).wait_send()

        @pl.when(me != ends[p])
        def _():
            cols_copy(p, 0).wait_recv()

    for p in range(pairs):
        s, h = divmod(p, heads)
        cache_ref[s, h] = cols_recv[p]

    each_other(lambda step, target: part_copy(step, target, rank).wait_send())

    for p in range(pairs):

        @pl.when(me == ends[p])
        def _():
            for d in range(sp_size):
                if d != ends[p]:
                    cols_copy(p, d).wait_send()

    @pl.when(me == last)
    def _():
        for p in peers:
            peer_copy(p).wait_send()

    @pl.when(me > meeting)
    def _():
        back_copy(me - 1).wait_send()

    @pl.when(me == meeting)
    def _():
        for d in range(sp_size):
            if d != meeting:
                norm_copy(d).wait_send()


def finish_kernel(cache_ref, out_ref, cache_out, out_out):
    cache_out[...] = bf(cache_ref[...])
    out_out[...] = out_ref[...]


def per_device(
    sp_size,
    tp_size,
    layer_input,
    key_weight,
    value_weight,
    beta_weight,
    beta_shift,
    decay_weight,
    decay_rate,
    decay_extra,
    query_new,
    gate_new,
    norm_gain,
    out_weight,
):
    seqs = layer_input.shape[0]
    heads = key_weight.shape[1] // DK
    head_total = beta_weight.shape[1]
    columns = out_weight.shape[1]
    devices = sp_size * tp_size
    features = out_weight.shape[2] // devices
    pairs = seqs * heads
    rows = -(-pairs // 8) * 8
    vmem = pl.BlockSpec(memory_space=pltpu.VMEM)
    anywhere = pl.BlockSpec(memory_space=pl.ANY)
    dma = pltpu.SemaphoreType.DMA
    states = jax.ShapeDtypeStruct((seqs, heads, columns, DK), F32)
    outs = jax.ShapeDtypeStruct((seqs, features), F32)
    cache, out = pl.pallas_call(
        functools.partial(mixer_kernel, sp_size, tp_size),
        in_specs=[anywhere] * 3 + [vmem] * 9,
        out_specs=(vmem, vmem),
        out_shape=(states, outs),
        scratch_shapes=[
            pltpu.VMEM(layer_input.shape, BF16),
            pltpu.VMEM(key_weight.shape, BF16),
            pltpu.VMEM(value_weight.shape, BF16),
            pltpu.VMEM((seqs, heads, 2 * DK, DK), F32),
            pltpu.VMEM((pairs, 2, DK // 2, DK), F32),
            pltpu.VMEM((pairs, 2, DK // 2, DK), F32),
            pltpu.VMEM((sp_size, pairs, columns, DK), F32),
            pltpu.VMEM((pairs, columns, DK), F32),
            pltpu.VMEM((2, rows, DK), F32),
            pltpu.VMEM((2, rows, DK), F32),
            pltpu.VMEM((rows, DK), F32),
            pltpu.VMEM((rows, DK), F32),
            pltpu.VMEM((devices, seqs, features), F32),
            pltpu.VMEM((devices, seqs, features), F32),
            pltpu.VMEM((seqs, heads, 2 * DK, DK), F32),
            dma((2 + seqs,)),
            dma((pairs, 2)),
            dma((pairs, 2)),
            dma((sp_size, pairs)),
            dma((pairs,)),
            dma((2,)),
            dma((sp_size,)),
            dma,
            dma((devices,)),
            dma((devices,)),
            dma((pairs,)),
            dma((pairs,)),
        ],
        compiler_params=pltpu.CompilerParams(
            collective_id=0, has_side_effects=True, vmem_limit_bytes=62 * 1024 * 1024
        ),
    )(
        layer_input,
        key_weight,
        value_weight,
        beta_weight.T,
        decay_weight.T,
        beta_shift.reshape(1, head_total),
        decay_rate.reshape(1, head_total),
        jnp.swapaxes(decay_extra, 1, 2),
        query_new,
        gate_new,
        norm_gain.reshape(1, DK),
        out_weight,
    )
    cache, out = pl.pallas_call(
        finish_kernel,
        in_specs=[vmem] * 2,
        out_specs=(vmem, vmem),
        out_shape=(jax.ShapeDtypeStruct(states.shape, BF16), outs),
    )(cache, out)
    return (jnp.swapaxes(cache, 2, 3), out)


def solution(mesh):
    return jax.shard_map(
        functools.partial(per_device, mesh.shape["sp"], mesh.shape["tp"]),
        mesh=mesh,
        in_specs=(
            P("grp", "sp", None),
            P(None, "tp"),
            P(None, "tp"),
            P(),
            P(),
            P(),
            P(),
            P("grp", "sp", "tp"),
            P("grp", "tp"),
            P("grp", "tp"),
            P(),
            P("tp", "sp", None),
        ),
        out_specs=(P("grp", "tp", None, "sp"), P("grp", ("sp", "tp"))),
        check_vma=False,
    )
```
